256 devices in a mesh: sp: 64 (over z, y, core), tp: 4 (over x).
Axes of the slice: x: 4, y: 4, z: 8, core: 2. Of those that a mesh axis runs over, the one named last changes fastest.
Arguments:
- tokens: bfloat16 [16384, 2048], P('sp', 'tp'), may hold values from -6 to 6
- in_gain: float32 [2048], replicated, may hold values from 0.1 to 1.9
- query_down: bfloat16 [2048, 512], replicated, may hold values from -0.125 to 0.125
- latent_down: bfloat16 [2048, 256], replicated, may hold values from -0.125 to 0.125
- rope_down: bfloat16 [2048, 32], replicated, may hold values from -0.125 to 0.125
- query_gain: float32 [512], replicated, may hold values from 0.5 to 12
- latent_gain: float32 [256], replicated, may hold values from 0.5 to 12
- query_nope: bfloat16 [512, 1024], P(None, 'tp'), may hold values from -0.25 to 0.25
- query_rope: bfloat16 [512, 512], P(None, 'tp'), may hold values from -0.25 to 0.25
- key_up: bfloat16 [256, 1024], P(None, 'tp'), may hold values from -0.375 to 0.375
- value_up: bfloat16 [256, 1024], P(None, 'tp'), may hold values from -0.375 to 0.375
- conv_value: bfloat16 [2048, 2048], P(None, 'tp'), may hold values from -0.125 to 0.125
- conv_gate: bfloat16 [2048, 2048], P(None, 'tp'), may hold values from -0.125 to 0.125
- conv_taps: float32 [31, 2048], P(None, 'tp'), may hold values from -1 to 1
- conv_bias: float32 [2048], P('tp'), may hold values from 0.05 to 2.25
- channel_gain: float32 [2048], P('tp'), may hold values from 0.1 to 1.9
- out_attend: bfloat16 [1024, 2048], P('tp'), may hold values from -0.109375 to 0.109375
- out_conv: bfloat16 [2048, 2048], P('tp'), may hold values from -0.109375 to 0.109375
Outputs:
- mixed: bfloat16 [16384, 2048], P('sp', 'tp')
The draws below stay inside these ranges and needn't reach their ends.
All inputs are finite; a program needn't handle non-finite values.
Results may differ from the reference program's by a relative error of at most 0.013.
The reference program's roundings to bfloat16 on the way count: a program that leaves them out, or rounds other values in their place, can miss the bound.
Values may be sent and summed in bfloat16 or wider, within the bound.
No kernel may reach another device: no remote copies, remote signals or barrier semaphores. Data moves between devices by JAX's collectives and lax.ppermute only.
A program may use at most 128 MiB of HBM per device.

```python
import math
import jax
import jax.numpy as jnp
from jax import lax

D = 2048
HEADS = 16
NOPE = 64
ROPE = 32
VDIM = 64
QRANK = 512
KVRANK = 256
CONV_CH = 2048
KWIDTH = 31
SEQ = 16384
GROUPS = 4


def draw_query_gain(key, part):
    return jax.random.uniform(key, (QRANK,), jnp.float32, 0.5, 1.5)


def draw_latent_gain(key, part):
    return jax.random.uniform(key, (KVRANK,), jnp.float32, 0.5, 1.5)


def draw_conv_bias(key, part):
    factor = jax.random.uniform(key, (CONV_CH,), jnp.float32, 0.5, 1.5)
    ramp = jnp.arange(CONV_CH).astype(jnp.float32) / (CONV_CH - 1)
    level = 0.1 + 0.9 * ramp
    return level * factor


def level_of(rng, extent, pieces, low, top_value):
    level, own = 1.0, jax.random.fold_in(rng, 6)
    for dim, blocks in pieces:
        draws = jnp.exp(jax.random.uniform(jax.random.fold_in(own, dim), (blocks,), jnp.float32, low / len(pieces), top_value / len(pieces)))
        level = level * jnp.repeat(draws, extent[dim] // blocks).reshape([-1 if axis == dim else 1 for axis in range(len(extent))])
    return level


def normal_values(rng, shape, deviation, most, shards=(), kind=jnp.bfloat16):
    result = deviation * jax.random.normal(rng, shape, jnp.float32)
    if shards:
        result = result * level_of(rng, shape, shards, -0.22, 0.18)
    return jnp.clip(result, -most, most).astype(kind)


def setup_inputs(seed: int = 0) -> dict:
    key_of = jax.random.split(jax.random.key(seed), 19)
    tokens = normal_values(key_of[0], (SEQ, D), 1.0, 6.0, ((0, 64), (1, 4)))
    in_gain = jnp.clip(1.0 + 0.18 * jax.random.normal(key_of[1], (D,), jnp.float32), 0.1, 1.9)
    query_down = normal_values(key_of[2], (D, QRANK), D ** -0.5, 0.125)
    latent_down = normal_values(key_of[3], (D, KVRANK), D ** -0.5, 0.125)
    rope_down = normal_values(key_of[4], (D, ROPE), D ** -0.5, 0.125)
    query_gain = draw_query_gain(jax.random.fold_in(key_of[18], 71), 0)
    latent_gain = draw_latent_gain(jax.random.fold_in(key_of[18], 71), 0)
    query_nope = normal_values(key_of[7], (QRANK, HEADS * NOPE), QRANK ** -0.5, 0.25, ((1, 4),))
    query_rope = normal_values(key_of[8], (QRANK, HEADS * ROPE), QRANK ** -0.5, 0.25, ((1, 4),))
    key_up = normal_values(key_of[9], (KVRANK, HEADS * NOPE), KVRANK ** -0.5, 0.375, ((1, 4),))
    value_up = normal_values(key_of[10], (KVRANK, HEADS * VDIM), KVRANK ** -0.5, 0.375, ((1, 4),))
    conv_value = normal_values(key_of[11], (D, CONV_CH), D ** -0.5, 0.125, ((1, 4),))
    conv_gate = normal_values(key_of[12], (D, CONV_CH), D ** -0.5, 0.125, ((1, 4),))
    conv_taps = normal_values(key_of[13], (KWIDTH, CONV_CH), KWIDTH ** -0.5, 1.0, ((1, 4),), jnp.float32)
    conv_bias = draw_conv_bias(jax.random.fold_in(key_of[18], 71), 0)
    channel_gain = jnp.clip(1.0 + 0.18 * jax.random.normal(key_of[15], (CONV_CH,), jnp.float32), 0.1, 1.9)
    out_attend = normal_values(key_of[16], (HEADS * VDIM, D), (HEADS * VDIM + CONV_CH) ** -0.5, 0.109375, ((0, 4),))
    out_conv = normal_values(key_of[17], (CONV_CH, D), (HEADS * VDIM + CONV_CH) ** -0.5, 0.109375, ((0, 4),))
    return dict(tokens=tokens, in_gain=in_gain, query_down=query_down, latent_down=latent_down, rope_down=rope_down, query_gain=query_gain, latent_gain=latent_gain, query_nope=query_nope, query_rope=query_rope, key_up=key_up, value_up=value_up, conv_value=conv_value, conv_gate=conv_gate, conv_taps=conv_taps, conv_bias=conv_bias, channel_gain=channel_gain, out_attend=out_attend, out_conv=out_conv)


eps_norm = 1e-06
eps_layer = 1e-05
theta = 10000.0

def rms_scale(values, gain):
    return values * lax.rsqrt(lax.optimization_barrier(jnp.mean(values * values, axis=-1, keepdims=True)) + eps_norm) * gain

def rotate(values, positions):
    half = values.shape[-1] // 2
    freqs = theta ** (-jnp.arange(half).astype(jnp.float32) / half)
    angles = positions[..., None] * freqs
    cosine = jnp.cos(angles)
    sine = jnp.sin(angles)
    first = values[..., :half]
    second = values[..., half:]
    return jnp.concatenate([first * cosine - second * sine, second * cosine + first * sine], axis=-1)

def reference(tokens, in_gain, query_down, latent_down, rope_down, query_gain, latent_gain, query_nope, query_rope, key_up, value_up, conv_value, conv_gate, conv_taps, conv_bias, channel_gain, out_attend, out_conv):
    tokens_f = tokens.astype(jnp.float32)
    row_scale = lax.rsqrt(lax.optimization_barrier(jnp.mean(tokens_f * tokens_f, axis=-1, keepdims=True)) + eps_norm)
    scaled = (tokens_f * in_gain).astype(jnp.bfloat16)
    positions = jnp.arange(SEQ).astype(jnp.float32)

    def project(weight):
        return row_scale * jnp.dot(scaled, weight, preferred_element_type=jnp.float32)
    q_latent = rms_scale(project(query_down), query_gain).astype(jnp.bfloat16)
    kv_latent = rms_scale(project(latent_down), latent_gain).astype(jnp.bfloat16)
    rope_key = rotate(project(rope_down), positions).astype(jnp.bfloat16)
    q_nope = jnp.dot(q_latent, query_nope, preferred_element_type=jnp.float32).astype(jnp.bfloat16)
    q_turn = jnp.dot(q_latent, query_rope, preferred_element_type=jnp.float32).reshape(SEQ, HEADS, ROPE)
    q_rope = rotate(q_turn, positions[:, None]).astype(jnp.bfloat16)
    k_nope = jnp.dot(kv_latent, key_up, preferred_element_type=jnp.float32).astype(jnp.bfloat16)
    values = jnp.dot(kv_latent, value_up, preferred_element_type=jnp.float32).astype(jnp.bfloat16)
    key_heads = k_nope.astype(jnp.float32).reshape(SEQ, HEADS, NOPE)
    value_heads = values.astype(jnp.float32).reshape(SEQ, HEADS, VDIM)
    rope_f = rope_key.astype(jnp.float32)
    score_scale = (NOPE + ROPE) ** (-0.5)
    block = math.gcd(SEQ, 256)
    q_blocks = q_nope.reshape(SEQ // block, block, HEADS, NOPE)
    r_blocks = q_rope.reshape(SEQ // block, block, HEADS, ROPE)

    def attend(pair):
        q_part = pair[0].astype(jnp.float32)
        r_part = pair[1].astype(jnp.float32)
        scores = (jnp.einsum('qhd,khd->hqk', q_part, key_heads) + jnp.einsum('qhd,kd->hqk', r_part, rope_f)) * score_scale
        highest = lax.optimization_barrier(jnp.max(scores, axis=-1, keepdims=True))
        weight = jnp.exp(scores - highest)
        total = lax.optimization_barrier(jnp.sum(weight, axis=-1))
        rounded = lax.optimization_barrier(weight.astype(jnp.bfloat16)).astype(jnp.float32)
        summed = jnp.einsum('hqk,khd->qhd', rounded, value_heads)
        return (summed / jnp.transpose(total)[:, :, None]).astype(jnp.bfloat16)
    attended = lax.map(attend, (q_blocks, r_blocks)).reshape(SEQ, HEADS * VDIM)
    glu = (project(conv_value) * jax.nn.sigmoid(project(conv_gate))).astype(jnp.bfloat16)
    half = KWIDTH // 2
    padded = jnp.pad(glu.astype(jnp.float32), ((half, half), (0, 0)))
    conv = jnp.zeros((SEQ, CONV_CH), jnp.float32) + conv_bias
    for tap in range(KWIDTH):
        conv = conv + conv_taps[tap] * padded[tap:tap + SEQ]
    mean = lax.optimization_barrier(jnp.mean(conv, axis=-1, keepdims=True))
    centred = conv - mean
    spread = lax.optimization_barrier(jnp.mean(centred * centred, axis=-1, keepdims=True))
    activated = jax.nn.silu(centred * lax.rsqrt(spread + eps_layer) * channel_gain).astype(jnp.bfloat16)
    head_cols = HEADS * VDIM // GROUPS
    chan_cols = CONV_CH // GROUPS
    mixed = jnp.zeros((SEQ, D), jnp.float32)
    for group in range(GROUPS):
        part_attend = jnp.dot(attended[:, group * head_cols:(group + 1) * head_cols], out_attend[group * head_cols:(group + 1) * head_cols], preferred_element_type=jnp.float32)
        part_conv = jnp.dot(activated[:, group * chan_cols:(group + 1) * chan_cols], out_conv[group * chan_cols:(group + 1) * chan_cols], preferred_element_type=jnp.float32)
        mixed = mixed + (part_attend + part_conv).astype(jnp.bfloat16).astype(jnp.float32)
    return mixed.astype(jnp.bfloat16)
```

```python
import functools
import math

import jax
import jax.numpy as jnp
from jax import lax
from jax.experimental import pallas as pl
from jax.experimental.pallas import tpu as pltpu
from jax.sharding import PartitionSpec as P


eps_norm = 1e-06
eps_layer = 1e-05
theta = 10000.0
Z, Y, C = 8, 4, 2
f32 = jnp.float32
bf16 = jnp.bfloat16
LANES = 128
EXTRA = 16


def moved(values, dz=0, dy=0, dc=0):
    pairs = []
    for z in range(Z):
        for y in range(Y):
            for c in range(C):
                to = (((z + dz) % Z) * Y + (y + dy) % Y) * C + (c + dc) % C
                pairs.append(((z * Y + y) * C + c, to))
    return lax.ppermute(values, "sp", pairs)


def passed_on(values):
    pairs = []
    for z in range(Z):
        for y in range(Y):
            for c in range(C):
                pairs.append(((z * Y + y) * C + c, (((z + 1 - 2 * c) % Z) * Y + y) * C + c))
    return lax.ppermute(values, "sp", pairs)


def moved_tp(values, step):
    count = lax.axis_size("tp")
    return lax.ppermute(values, "tp", [(i, (i + step) % count) for i in range(count)])


def in_order(me, came):
    ordered = []
    for j in range(4):
        k = lax.rem(j - me + 4, 4)
        ordered.append(
            jnp.where(k == 0, came[0], jnp.where(k == 1, came[1], jnp.where(k == 2, came[2], came[3])))
        )
    return ordered


def prepare_kernel(heads, key_up, value_up, kup, vup, place):
    nope = key_up.shape[1] // heads
    gap = jnp.zeros((key_up.shape[0], LANES - nope), bf16)
    for h in range(heads):
        kup[:, h * LANES : (h + 1) * LANES] = jnp.concatenate(
            [key_up[:, h * nope : (h + 1) * nope], gap], axis=1
        )
    vup[...] = jnp.transpose(value_up[...])
    row = lax.broadcasted_iota(jnp.int32, place.shape, 0)
    column = lax.broadcasted_iota(jnp.int32, place.shape, 1)
    place[...] = jnp.where(column == row + nope, 1.0, 0.0).astype(bf16)


def prepare(key_up, value_up, heads, rope_size):
    vmem = pl.BlockSpec(memory_space=pltpu.VMEM)
    return pl.pallas_call(
        functools.partial(prepare_kernel, heads),
        out_shape=(
            jax.ShapeDtypeStruct((key_up.shape[0], heads * LANES), bf16),
            jax.ShapeDtypeStruct(value_up.shape[::-1], bf16),
            jax.ShapeDtypeStruct((rope_size, LANES), bf16),
        ),
        in_specs=[vmem] * 2,
        out_specs=(vmem,) * 3,
        cost_estimate=pl.CostEstimate(flops=10**7, bytes_accessed=10**6, transcendentals=0),
        compiler_params=pltpu.CompilerParams(vmem_limit_bytes=8 * 2**20),
        name="prepare",
    )(key_up, value_up)


def attend_kernel(sizes, nq, heads, first, last, scale, skip, *refs):
    nl = len(sizes)
    lat = [refs[k].at[j] for k, size in enumerate(sizes) for j in range(size)]
    kup, vup, place = refs[nl : nl + 3]
    q = refs[nl + 3 : nl + 3 + nq]
    at = nl + 3 + nq
    if not first:
        state, high = refs[at : at + 2]
        at += 2
    if last:
        out = refs[at]
        at += 1
    else:
        out, out_high = refs[at : at + 2]
        at += 2
    kbuf, vbuf, qbuf, sa, sb, pa, pb, ma, mb, tops = refs[at:]
    keys = lat[0].shape[1]
    rank = kup.shape[0]
    vdim = vup.shape[0] // heads
    n = len(lat) * keys
    items = nq * heads
    dq = q[0].shape[0] // heads
    for b, ref in enumerate(lat):
        block = ref[:rank]
        rope = lax.dot_general(
            ref[rank:], place[...], (((0,), (0,)), ((), ())), preferred_element_type=f32
        )
        kk = jnp.dot(block, kup[...], preferred_element_type=f32)
        vv = lax.dot_general(vup[...], block, (((1,), (1,)), ((), ())), preferred_element_type=f32)
        rows = slice(b * keys, (b + 1) * keys)
        for h in range(heads):
            kbuf[h, rows, :] = (kk[:, h * LANES : (h + 1) * LANES] + rope).astype(bf16)
            vbuf[h, :vdim, rows] = vv[h * vdim : (h + 1) * vdim].astype(bf16)
    for h in range(heads):
        vbuf[h, vdim:, :] = jnp.ones((vbuf.shape[1] - vdim, n), bf16)
    for i in range(nq):
        for h in range(heads):
            qbuf[i * heads + h, :dq, :] = q[i][h * dq : (h + 1) * dq]
            qbuf[i * heads + h, dq:, :] = jnp.zeros((LANES - dq, q[i].shape[1]), bf16)

    def scores(i, s_ref, m_ref):
        s = jnp.dot(kbuf[lax.rem(i, heads)], qbuf[i], preferred_element_type=f32) * scale
        s_ref[...] = s
        top = jnp.max(s, axis=0, keepdims=True)
        if not first:
            before = high[i + skip][:1]
            top = jnp.maximum(top, before)
        top = top.astype(bf16).astype(f32)
        shrink = top if first else jnp.exp2(before - top)
        m_ref[...] = jnp.broadcast_to(top, m_ref.shape)
        tops[i] = jnp.concatenate([jnp.broadcast_to(v, (8, v.shape[1])) for v in (top, shrink)])

    def weights(s_ref, m_ref, p_ref):
        p_ref[...] = jnp.exp2(s_ref[...] - m_ref[:1]).astype(bf16)

    def values(i, p_ref):
        o = jnp.dot(vbuf[lax.rem(i, heads)], p_ref[...], preferred_element_type=f32)
        top = tops[i, :8]
        if not first:
            o = o + state[i + skip] * tops[i, 8:9]
        if not last:
            out[i] = o
            out_high[i] = top
            return
        total = o[vdim : vdim + 8]
        total_high = total.astype(bf16).astype(f32)
        row = lax.broadcasted_iota(jnp.int32, total.shape, 0)
        tail = jnp.where(row == 0, total_high, jnp.where(row == 1, total - total_high, top))
        out[i] = jnp.concatenate([o[:vdim], tail, tail], axis=0).astype(bf16)

    scores(0, sa, ma)
    scores(1, sb, mb)
    weights(sa, ma, pa)

    def step(j, carry):
        i = 2 * j
        scores(i + 2, sa, ma)
        weights(sb, mb, pb)
        values(i, pa)
        scores(i + 3, sb, mb)
        weights(sa, ma, pa)
        values(i + 1, pb)
        return carry

    lax.fori_loop(0, items // 2 - 1, step, 0)
    weights(sb, mb, pb)
    values(items - 2, pa)
    values(items - 1, pb)


def attend(lat, kup, vup, place, q, heads, scale, state=None, last=False, skip=0):
    nq = len(q)
    sizes = [item.shape[0] for item in lat]
    keys, toks = lat[0].shape[2], q[0].shape[1]
    n = sum(sizes) * keys
    rows = vup.shape[0] // heads + EXTRA
    items = nq * heads
    first = state is None
    args = [*lat, kup, vup, place, *q] + ([] if first else list(state))
    vmem = pl.BlockSpec(memory_space=pltpu.VMEM)
    if last:
        out_shape = (jax.ShapeDtypeStruct((items, rows, toks), bf16),)
    else:
        out_shape = (
            jax.ShapeDtypeStruct((items, rows, toks), f32),
            jax.ShapeDtypeStruct((items, 8, toks), f32),
        )
    return pl.pallas_call(
        functools.partial(attend_kernel, sizes, nq, heads, first, last, scale, skip),
        out_shape=out_shape,
        in_specs=[vmem] * len(args),
        out_specs=(vmem,) * len(out_shape),
        scratch_shapes=[
            pltpu.VMEM((heads, n, LANES), bf16),
            pltpu.VMEM((heads, rows, n), bf16),
            pltpu.VMEM((items, LANES, toks), bf16),
            pltpu.VMEM((n, toks), f32),
            pltpu.VMEM((n, toks), f32),
            pltpu.VMEM((n, toks), bf16),
            pltpu.VMEM((n, toks), bf16),
            pltpu.VMEM((8, toks), f32),
            pltpu.VMEM((8, toks), f32),
            pltpu.VMEM((items, 16, toks), f32),
        ],
        cost_estimate=pl.CostEstimate(
            flops=2 * items * toks * n * 336, bytes_accessed=4 * 2**20, transcendentals=items * toks * n
        ),
        compiler_params=pltpu.CompilerParams(vmem_limit_bytes=24 * 2**20),
        name="attend",
    )(*args)


def merge_kernel(heads, me, *refs):
    parts = refs[:4]
    w_ref, conv_ref = refs[4:6]
    outs = refs[6:10]
    rows, toks = parts[0].shape[1:]
    vdim = rows - EXTRA
    columns = []
    for h in range(heads):
        tops = [p[h, vdim + 2 : vdim + 3].astype(f32) for p in parts]
        top = functools.reduce(jnp.maximum, tops)
        total = jnp.zeros((1, toks), f32)
        sums = jnp.zeros((vdim, toks), f32)
        for p, t in zip(parts, tops):
            factor = jnp.exp2(t - top)
            ends = p[h, vdim : vdim + 2].astype(f32)
            total = total + (ends[:1] + ends[1:]) * factor
            sums = sums + p[h, :vdim].astype(f32) * factor
        columns.append((sums / total).astype(bf16))
    attended = jnp.concatenate(columns, axis=0)
    feats = outs[0].shape[1]
    for k in range(4):
        at = pl.multiple_of(lax.rem(me[0] + k, 4) * feats, feats)
        part = lax.dot_general(
            attended, w_ref[:, pl.ds(at, feats)], (((0,), (0,)), ((), ())), preferred_element_type=f32
        )
        outs[k][...] = (part + conv_ref[:, pl.ds(at, feats)]).astype(bf16)


def merge(me, parts, out_attend, conv_part):
    heads, _, toks = parts[0].shape
    vmem = pl.BlockSpec(memory_space=pltpu.VMEM)
    shape = jax.ShapeDtypeStruct((toks, out_attend.shape[1] // 4), bf16)
    return pl.pallas_call(
        functools.partial(merge_kernel, heads),
        out_shape=(shape,) * 4,
        in_specs=[pl.BlockSpec(memory_space=pltpu.SMEM)] + [vmem] * 6,
        out_specs=(vmem,) * 4,
        cost_estimate=pl.CostEstimate(
            flops=2 * toks * out_attend.size, bytes_accessed=5 * 2**20, transcendentals=0
        ),
        compiler_params=pltpu.CompilerParams(vmem_limit_bytes=16 * 2**20),
        name="merge",
    )(jnp.reshape(me, (1,)).astype(jnp.int32), *parts, out_attend, conv_part)


def rms_scale(values, gain):
    return values * lax.rsqrt(jnp.mean(values * values, axis=-1, keepdims=True) + eps_norm) * gain


def rotate_rows(values, positions):
    half = values.shape[-2] // 2
    freqs = theta ** (-jnp.arange(half).astype(f32) / half)
    angles = freqs[:, None] * positions
    cosine = jnp.cos(angles)
    sine = jnp.sin(angles)
    first = values[..., :half, :]
    second = values[..., half:, :]
    return jnp.concatenate(
        [first * cosine - second * sine, second * cosine + first * sine], axis=-2
    )


def columns(weight, rows):
    return lax.dot_general(weight, rows, (((0,), (1,)), ((), ())), preferred_element_type=f32)


def per_device(
    tokens,
    in_gain,
    query_down,
    latent_down,
    rope_down,
    query_gain,
    latent_gain,
    query_nope,
    query_rope,
    key_up,
    value_up,
    conv_value,
    conv_gate,
    conv_taps,
    conv_bias,
    channel_gain,
    out_attend,
    out_conv,
):
    row_count = tokens.shape[0]
    width = in_gain.shape[0]
    local_ch = conv_value.shape[1]
    sp = lax.axis_index("sp")
    positions = (sp * row_count + jnp.arange(row_count)).astype(f32)
    rope_size = rope_down.shape[1]
    heads = query_rope.shape[1] // rope_size
    nope = key_up.shape[1] // heads
    score_scale = (nope + rope_size) ** -0.5 * math.log2(math.e)

    me = lax.axis_index("tp")
    came = [tokens] + [moved_tp(tokens, step) for step in (-1, 2, 1)]
    piece_f = jnp.concatenate(in_order(me, came), axis=1).astype(f32)
    scaled = (piece_f * in_gain).astype(bf16)
    square_sum = jnp.sum(piece_f * piece_f, axis=1)
    row_scale = lax.rsqrt(square_sum / width + eps_norm)[:, None]

    def add_rows(weight):
        return jnp.dot(scaled, weight, preferred_element_type=f32)

    kv_latent = rms_scale(row_scale * add_rows(latent_down), latent_gain).astype(bf16)
    rope_key = rotate_rows(columns(rope_down, scaled) * row_scale[:, 0], positions).astype(bf16)
    lat = jnp.concatenate([kv_latent, rope_key], axis=0)
    q_latent = rms_scale(row_scale * add_rows(query_down), query_gain).astype(bf16)
    q_flat = columns(query_nope, q_latent).astype(bf16).reshape(heads, nope, row_count)
    q_turn = columns(query_rope, q_latent).reshape(heads, rope_size, row_count)
    r_flat = rotate_rows(q_turn, positions).astype(bf16)
    q_own = jnp.concatenate([q_flat, r_flat], axis=1).reshape(heads * (nope + rope_size), row_count)

    q_far = [moved(q_own, dy=d) for d in (1, -1, 2)]

    own = jnp.stack([lat, moved(lat, dc=1)])
    hop1 = passed_on(own)
    hop2 = passed_on(hop1)
    hop3 = passed_on(hop2)
    hop4 = passed_on(hop3[:1])
    side1, side2, side3, side4 = (
        moved(hop, dc=1) for hop in (hop1, hop2, hop3, hop4)
    )

    kup, vup, place = prepare(key_up, value_up, heads, rope_size)

    def part(blocks, queries, state=None, last=False, skip=0):
        return attend(
            blocks, kup, vup, place, queries, heads, score_scale, state, last, skip
        )

    glu = (
        row_scale * add_rows(conv_value) * jax.nn.sigmoid(row_scale * add_rows(conv_gate))
    ).astype(bf16)
    taps = conv_taps.shape[0]
    reach = taps // 2
    count = lax.axis_size("sp")
    before = lax.ppermute(glu[row_count - reach :], "sp", [(i, i + 1) for i in range(count - 1)])
    after = lax.ppermute(glu[:reach], "sp", [(i + 1, i) for i in range(count - 1)])
    padded = jnp.concatenate([before, glu, after], axis=0).astype(f32)
    conv = jnp.zeros((row_count, local_ch), f32) + conv_bias
    for tap in range(taps):
        conv = conv + conv_taps[tap] * padded[tap : tap + row_count]
    own_mean = jnp.mean(conv, axis=-1)
    own_off = conv - own_mean[:, None]
    own_stats = jnp.stack([own_mean, jnp.sum(own_off * own_off, axis=-1)])
    stats = jnp.stack([own_stats] + [moved_tp(own_stats, k) for k in (1, -1, 2)])
    mean = jnp.mean(stats[:, 0], axis=0)
    apart = stats[:, 0] - mean
    spread = jnp.sum(stats[:, 1] + local_ch * apart * apart, axis=0) / (4 * local_ch)
    activated = jax.nn.silu(
        (conv - mean[:, None]) * lax.rsqrt(spread + eps_layer)[:, None] * channel_gain
    ).astype(bf16)

    conv_part = jnp.dot(activated, out_conv, preferred_element_type=f32)

    own_first = [q_own] + q_far
    state = part([own, hop1], own_first)
    state = part([side1, hop2], own_first, state)
    state = part([side2, hop3], own_first, state)
    ends = [side3, hop4, side4]
    (packed,) = part(ends, q_far, state, True, heads)
    packed = packed.reshape((3, heads) + packed.shape[1:])

    parts = [moved(packed[k], dy=d) for k, d in enumerate((-1, 1, 2))]
    (packed_own,) = part(ends, [q_own], state, True)
    cuts = merge(me, [packed_own] + parts, out_attend, conv_part)
    mixed = cuts[0].astype(f32)
    for k, step in ((1, 1), (2, 2), (3, -1)):
        mixed = mixed + moved_tp(cuts[k], step).astype(f32)
    return mixed.astype(bf16)


def solution(mesh):
    in_specs = (
        P("sp", "tp"),
        P(),
        P(),
        P(),
        P(),
        P(),
        P(),
        P(None, "tp"),
        P(None, "tp"),
        P(None, "tp"),
        P(None, "tp"),
        P(None, "tp"),
        P(None, "tp"),
        P(None, "tp"),
        P("tp"),
        P("tp"),
        P("tp", None),
        P("tp", None),
    )
    out_specs = P("sp", "tp")


    return jax.shard_map(
        per_device, mesh=mesh, in_specs=in_specs, out_specs=out_specs, check_vma=False
    )
```

```python
import functools
import math

import jax
import jax.numpy as jnp
from jax import lax
from jax.experimental import pallas as pl
from jax.experimental.pallas import tpu as pltpu
from jax.sharding import PartitionSpec as P


eps_norm = 1e-06
eps_layer = 1e-05
theta = 10000.0
Z, Y, C = 8, 4, 2
f32 = jnp.float32
bf16 = jnp.bfloat16
LANES = 128
EXTRA = 16


def moved(values, dz=0, dy=0, dc=0):
    pairs = []
    for z in range(Z):
        for y in range(Y):
            for c in range(C):
                to = (((z + dz) % Z) * Y + (y + dy) % Y) * C + (c + dc) % C
                pairs.append(((z * Y + y) * C + c, to))
    return lax.ppermute(values, "sp", pairs)


def passed_on(values):
    pairs = []
    for z in range(Z):
        for y in range(Y):
            for c in range(C):
                pairs.append(((z * Y + y) * C + c, (((z + 1 - 2 * c) % Z) * Y + y) * C + c))
    return lax.ppermute(values, "sp", pairs)


def moved_tp(values, step):
    count = lax.axis_size("tp")
    return lax.ppermute(values, "tp", [(i, (i + step) % count) for i in range(count)])


def over_edge(values):
    count = lax.axis_size("sp")
    pairs = [(i, i + 1 if i % 2 else i - 1) for i in range(count) if 0 < i < count - 1]
    return lax.ppermute(values, "sp", pairs)


def in_order(me, came):
    ordered = []
    for j in range(4):
        k = lax.rem(j - me + 4, 4)
        ordered.append(
            jnp.where(k == 0, came[0], jnp.where(k == 1, came[1], jnp.where(k == 2, came[2], came[3])))
        )
    return ordered


def prepare_kernel(heads, key_up, value_up, kup, vup, place):
    nope = key_up.shape[1] // heads
    gap = jnp.zeros((key_up.shape[0], LANES - nope), bf16)
    for h in range(heads):
        kup[:, h * LANES : (h + 1) * LANES] = jnp.concatenate(
            [key_up[:, h * nope : (h + 1) * nope], gap], axis=1
        )
    vup[...] = jnp.transpose(value_up[...])
    row = lax.broadcasted_iota(jnp.int32, place.shape, 0)
    column = lax.broadcasted_iota(jnp.int32, place.shape, 1)
    place[...] = jnp.where(column == row + nope, 1.0, 0.0).astype(bf16)


def prepare(key_up, value_up, heads, rope_size):
    vmem = pl.BlockSpec(memory_space=pltpu.VMEM)
    return pl.pallas_call(
        functools.partial(prepare_kernel, heads),
        out_shape=(
            jax.ShapeDtypeStruct((key_up.shape[0], heads * LANES), bf16),
            jax.ShapeDtypeStruct(value_up.shape[::-1], bf16),
            jax.ShapeDtypeStruct((rope_size, LANES), bf16),
        ),
        in_specs=[vmem] * 2,
        out_specs=(vmem,) * 3,
        cost_estimate=pl.CostEstimate(flops=10**7, bytes_accessed=10**6, transcendentals=0),
        compiler_params=pltpu.CompilerParams(vmem_limit_bytes=8 * 2**20),
        name="prepare",
    )(key_up, value_up)


def attend_kernel(sizes, nq, heads, first, last, scale, skip, *refs):
    nl = len(sizes)
    lat = [refs[k].at[j] for k, size in enumerate(sizes) for j in range(size)]
    kup, vup, place = refs[nl : nl + 3]
    q = refs[nl + 3 : nl + 3 + nq]
    at = nl + 3 + nq
    if not first:
        state, high = refs[at : at + 2]
        at += 2
    if last:
        out = refs[at]
        at += 1
    else:
        out, out_high = refs[at : at + 2]
        at += 2
    kbuf, vbuf, qbuf, sa, sb, pa, pb, ma, mb, tops = refs[at:]
    keys = lat[0].shape[1]
    rank = kup.shape[0]
    vdim = vup.shape[0] // heads
    n = len(lat) * keys
    items = nq * heads
    dq = q[0].shape[0] // heads
    for b, ref in enumerate(lat):
        block = ref[:rank]
        rope = lax.dot_general(
            ref[rank:], place[...], (((0,), (0,)), ((), ())), preferred_element_type=f32
        )
        kk = jnp.dot(block, kup[...], preferred_element_type=f32)
        vv = lax.dot_general(vup[...], block, (((1,), (1,)), ((), ())), preferred_element_type=f32)
        rows = slice(b * keys, (b + 1) * keys)
        for h in range(heads):
            kbuf[h, rows, :] = (kk[:, h * LANES : (h + 1) * LANES] + rope).astype(bf16)
            vbuf[h, :vdim, rows] = vv[h * vdim : (h + 1) * vdim].astype(bf16)
    for h in range(heads):
        vbuf[h, vdim:, :] = jnp.ones((vbuf.shape[1] - vdim, n), bf16)
    for i in range(nq):
        for h in range(heads):
            qbuf[i * heads + h, :dq, :] = q[i][h * dq : (h + 1) * dq]
            qbuf[i * heads + h, dq:, :] = jnp.zeros((LANES - dq, q[i].shape[1]), bf16)

    def scores(i, s_ref, m_ref):
        s = jnp.dot(kbuf[lax.rem(i, heads)], qbuf[i], preferred_element_type=f32) * scale
        s_ref[...] = s
        top = jnp.max(s, axis=0, keepdims=True)
        if not first:
            before = high[i + skip][:1]
            top = jnp.maximum(top, before)
        top = top.astype(bf16).astype(f32)
        shrink = top if first else jnp.exp2(before - top)
        m_ref[...] = jnp.broadcast_to(top, m_ref.shape)
        tops[i] = jnp.concatenate([jnp.broadcast_to(v, (8, v.shape[1])) for v in (top, shrink)])

    def weights(s_ref, m_ref, p_ref):
        p_ref[...] = jnp.exp2(s_ref[...] - m_ref[:1]).astype(bf16)

    def values(i, p_ref):
        o = jnp.dot(vbuf[lax.rem(i, heads)], p_ref[...], preferred_element_type=f32)
        top = tops[i, :8]
        if not first:
            o = o + state[i + skip] * tops[i, 8:9]
        if not last:
            out[i] = o
            out_high[i] = top
            return
        total = o[vdim : vdim + 8]
        total_high = total.astype(bf16).astype(f32)
        row = lax.broadcasted_iota(jnp.int32, total.shape, 0)
        tail = jnp.where(row == 0, total_high, jnp.where(row == 1, total - total_high, top))
        out[i] = jnp.concatenate([o[:vdim], tail, tail], axis=0).astype(bf16)

    def score_pair(i):
        scores(i, sa, ma)
        scores(i + 1, sb, mb)

    def weight_pair():
        weights(sa, ma, pa)
        weights(sb, mb, pb)

    def value_pair(i):
        values(i, pa)
        values(i + 1, pb)

    score_pair(0)
    weight_pair()
    score_pair(2)

    def step(j, carry):
        value_pair(2 * j)
        weight_pair()
        score_pair(2 * j + 4)
        return carry

    lax.fori_loop(0, items // 2 - 2, step, 0)
    value_pair(items - 4)
    weight_pair()
    value_pair(items - 2)


def attend(lat, kup, vup, place, q, heads, scale, state=None, last=False, skip=0):
    nq = len(q)
    sizes = [item.shape[0] for item in lat]
    keys, toks = lat[0].shape[2], q[0].shape[1]
    n = sum(sizes) * keys
    rows = vup.shape[0] // heads + EXTRA
    items = nq * heads
    first = state is None
    args = [*lat, kup, vup, place, *q] + ([] if first else list(state))
    vmem = pl.BlockSpec(memory_space=pltpu.VMEM)
    if last:
        out_shape = (jax.ShapeDtypeStruct((items, rows, toks), bf16),)
    else:
        out_shape = (
            jax.ShapeDtypeStruct((items, rows, toks), f32),
            jax.ShapeDtypeStruct((items, 8, toks), f32),
        )
    return pl.pallas_call(
        functools.partial(attend_kernel, sizes, nq, heads, first, last, scale, skip),
        out_shape=out_shape,
        in_specs=[vmem] * len(args),
        out_specs=(vmem,) * len(out_shape),
        scratch_shapes=[
            pltpu.VMEM((heads, n, LANES), bf16),
            pltpu.VMEM((heads, rows, n), bf16),
            pltpu.VMEM((items, LANES, toks), bf16),
            pltpu.VMEM((n, toks), f32),
            pltpu.VMEM((n, toks), f32),
            pltpu.VMEM((n, toks), bf16),
            pltpu.VMEM((n, toks), bf16),
            pltpu.VMEM((8, toks), f32),
            pltpu.VMEM((8, toks), f32),
            pltpu.VMEM((items, 16, toks), f32),
        ],
        cost_estimate=pl.CostEstimate(
            flops=2 * items * toks * n * 336, bytes_accessed=4 * 2**20, transcendentals=items * toks * n
        ),
        compiler_params=pltpu.CompilerParams(vmem_limit_bytes=24 * 2**20),
        name="attend",
    )(*args)


def merge_kernel(heads, me, *refs):
    parts = refs[:4]
    w_ref, conv_ref = refs[4:6]
    outs = refs[6:10]
    rows, toks = parts[0].shape[1:]
    vdim = rows - EXTRA
    columns = []
    for h in range(heads):
        tops = [p[h, vdim + 2 : vdim + 3].astype(f32) for p in parts]
        top = functools.reduce(jnp.maximum, tops)
        total = jnp.zeros((1, toks), f32)
        sums = jnp.zeros((vdim, toks), f32)
        for p, t in zip(parts, tops):
            factor = jnp.exp2(t - top)
            ends = p[h, vdim : vdim + 2].astype(f32)
            total = total + (ends[:1] + ends[1:]) * factor
            sums = sums + p[h, :vdim].astype(f32) * factor
        columns.append((sums / total).astype(bf16))
    attended = jnp.concatenate(columns, axis=0)
    feats = outs[0].shape[1]
    for k in range(4):
        at = pl.multiple_of(lax.rem(me[0] + k, 4) * feats, feats)
        part = lax.dot_general(
            attended, w_ref[:, pl.ds(at, feats)], (((0,), (0,)), ((), ())), preferred_element_type=f32
        )
        outs[k][...] = (part + conv_ref[:, pl.ds(at, feats)]).astype(bf16)


def merge(me, parts, out_attend, conv_part):
    heads, _, toks = parts[0].shape
    vmem = pl.BlockSpec(memory_space=pltpu.VMEM)
    shape = jax.ShapeDtypeStruct((toks, out_attend.shape[1] // 4), bf16)
    return pl.pallas_call(
        functools.partial(merge_kernel, heads),
        out_shape=(shape,) * 4,
        in_specs=[pl.BlockSpec(memory_space=pltpu.SMEM)] + [vmem] * 6,
        out_specs=(vmem,) * 4,
        cost_estimate=pl.CostEstimate(
            flops=2 * toks * out_attend.size, bytes_accessed=5 * 2**20, transcendentals=0
        ),
        compiler_params=pltpu.CompilerParams(vmem_limit_bytes=16 * 2**20),
        name="merge",
    )(jnp.reshape(me, (1,)).astype(jnp.int32), *parts, out_attend, conv_part)


def rms_scale(values, gain):
    return values * lax.rsqrt(jnp.mean(values * values, axis=-1, keepdims=True) + eps_norm) * gain


def rotate_rows(values, positions):
    half = values.shape[-2] // 2
    freqs = theta ** (-jnp.arange(half).astype(f32) / half)
    angles = freqs[:, None] * positions
    cosine = jnp.cos(angles)
    sine = jnp.sin(angles)
    first = values[..., :half, :]
    second = values[..., half:, :]
    return jnp.concatenate(
        [first * cosine - second * sine, second * cosine + first * sine], axis=-2
    )


def columns(weight, rows):
    return lax.dot_general(weight, rows, (((0,), (1,)), ((), ())), preferred_element_type=f32)


def per_device(
    tokens,
    in_gain,
    query_down,
    latent_down,
    rope_down,
    query_gain,
    latent_gain,
    query_nope,
    query_rope,
    key_up,
    value_up,
    conv_value,
    conv_gate,
    conv_taps,
    conv_bias,
    channel_gain,
    out_attend,
    out_conv,
):
    row_count = tokens.shape[0]
    width = in_gain.shape[0]
    local_ch = conv_value.shape[1]
    sp = lax.axis_index("sp")
    positions = (sp * row_count + jnp.arange(row_count)).astype(f32)
    rope_size = rope_down.shape[1]
    heads = query_rope.shape[1] // rope_size
    nope = key_up.shape[1] // heads
    score_scale = (nope + rope_size) ** -0.5 * math.log2(math.e)

    me = lax.axis_index("tp")
    taps = conv_taps.shape[0]
    reach = taps // 2
    edge = (reach + 15) // 16 * 16

    def gathered(own):
        came = [own] + [moved_tp(own, step) for step in (-1, 2, 1)]
        return jnp.concatenate(in_order(me, came), axis=1).astype(f32)

    def normed(piece):
        return (piece * in_gain).astype(bf16), lax.rsqrt(
            jnp.sum(piece * piece, axis=1) / width + eps_norm
        )[:, None]

    whole = gathered(tokens)
    scaled, row_scale = normed(whole)

    even = lax.rem(sp, 2) == 0
    head, tail = tokens[:edge], tokens[row_count - edge :]
    near = moved(jnp.where(even, tail, head), dc=1)
    across = over_edge(jnp.where(even, head, tail))
    ends = jnp.concatenate([jnp.where(even, across, near), jnp.where(even, near, across)], axis=0)
    scaled_ends, scale_ends = normed(gathered(ends))

    def add_rows(weight):
        return jnp.dot(scaled, weight, preferred_element_type=f32)

    kv_latent = rms_scale(row_scale * add_rows(latent_down), latent_gain).astype(bf16)
    rope_key = rotate_rows(columns(rope_down, scaled) * row_scale[:, 0], positions).astype(bf16)
    lat = jnp.concatenate([kv_latent, rope_key], axis=0)
    q_pre = add_rows(query_down)
    q_latent = rms_scale(row_scale * q_pre, query_gain).astype(bf16)
    q_flat = columns(query_nope, q_latent).astype(bf16).reshape(heads, nope, row_count)
    q_turn = columns(query_rope, q_latent).reshape(heads, rope_size, row_count)
    r_flat = rotate_rows(q_turn, positions).astype(bf16)
    q_own = jnp.concatenate([q_flat, r_flat], axis=1).reshape(heads * (nope + rope_size), row_count)

    q_far = [moved(q_own, dy=d) for d in (1, -1, 2)]

    own = jnp.stack([lat, moved(lat, dc=1)])
    hop1 = passed_on(own)
    hop2 = passed_on(hop1)
    hop3 = passed_on(hop2)
    hop4 = passed_on(hop3[:1])
    side1, side2, side3, side4 = (
        moved(hop, dc=1) for hop in (hop1, hop2, hop3, hop4)
    )

    kup, vup, place = prepare(key_up, value_up, heads, rope_size)

    def part(blocks, queries, state=None, last=False, skip=0):
        return attend(
            blocks, kup, vup, place, queries, heads, score_scale, state, last, skip
        )

    wide = jnp.concatenate([scaled_ends[:edge], scaled, scaled_ends[edge:]], axis=0)
    wide_scale = jnp.concatenate([scale_ends[:edge], row_scale, scale_ends[edge:]], axis=0)
    glu = (
        wide_scale
        * jnp.dot(wide, conv_value, preferred_element_type=f32)
        * jax.nn.sigmoid(wide_scale * jnp.dot(wide, conv_gate, preferred_element_type=f32))
    )
    glu = lax.reduce_precision(glu, 8, 7)
    padded = glu[edge - reach : edge + row_count + reach]
    conv = jnp.zeros((row_count, local_ch), f32) + conv_bias
    for tap in range(taps):
        conv = conv + conv_taps[tap] * padded[tap : tap + row_count]
    own_mean = jnp.mean(conv, axis=-1)
    own_off = conv - own_mean[:, None]
    own_square = jnp.sum(own_off * own_off, axis=-1)
    mean, square, channels = own_mean, own_square, local_ch
    for step in (1, 2):
        pairs = [(i, i ^ step) for i in range(4)]
        other = lax.ppermute(jnp.stack([mean, square]), "tp", pairs)
        apart = other[0] - mean
        mean = (mean + other[0]) * 0.5
        square = square + other[1] + apart * apart * (channels * 0.5)
        channels *= 2
    spread = square / channels
    activated = jax.nn.silu(
        (conv - mean[:, None]) * lax.rsqrt(spread + eps_layer)[:, None] * channel_gain
    ).astype(bf16)

    conv_part = jnp.dot(activated, out_conv, preferred_element_type=f32)

    own_first = [q_own] + q_far
    state = part([own, hop1], own_first)
    state = part([side1, hop2], own_first, state)
    state = part([side2, hop3], own_first, state)
    rest = [side3, hop4, side4]
    (packed,) = part(rest, q_far, state, True, heads)
    packed = packed.reshape((3, heads) + packed.shape[1:])

    parts = [moved(packed[k], dy=d) for k, d in enumerate((-1, 1, 2))]
    (packed_own,) = part(rest, [q_own], state, True)
    cuts = merge(me, [packed_own] + parts, out_attend, conv_part)
    mixed = cuts[0].astype(f32)
    for k, step in ((1, 1), (2, 2), (3, -1)):
        mixed = mixed + moved_tp(cuts[k], step).astype(f32)
    return mixed.astype(bf16)


def solution(mesh):
    in_specs = (
        P("sp", "tp"),
        P(),
        P(),
        P(),
        P(),
        P(),
        P(),
        P(None, "tp"),
        P(None, "tp"),
        P(None, "tp"),
        P(None, "tp"),
        P(None, "tp"),
        P(None, "tp"),
        P(None, "tp"),
        P("tp"),
        P("tp"),
        P("tp", None),
        P("tp", None),
    )
    out_specs = P("sp", "tp")


    return jax.shard_map(
        per_device, mesh=mesh, in_specs=in_specs, out_specs=out_specs, check_vma=False
    )
```
